32 devices in a mesh: grp: 2 (over y), sp: 4 (over z), tp: 4 (over x, core).
Axes of the slice: x: 2, y: 2, z: 4, core: 2. Of those that a mesh axis runs over, the one named last changes fastest.
Arguments:
- query_rows: bfloat16 [1024, 1024], P(('grp', 'sp'), 'tp'), parts along dimension 0, may hold values from -12 to 12
- key_rows: bfloat16 [1024, 1024], P(('grp', 'sp'), 'tp'), parts along dimension 0, may hold values from -9 to 9
- value_rows: bfloat16 [1024, 1024], P(('grp', 'sp'), 'tp'), parts along dimension 0, may hold values from -6 to 6
- key_logit: bfloat16 [1024, 8], P(('grp', 'sp'), 'tp'), parts along dimension 0, as said below
- residual: bfloat16 [1024, 2048], P(('grp', 'sp')), parts along dimension 0, may hold values from -6 to 6
- out_weight: bfloat16 [1024, 2048], P('tp'), may hold values from -0.1875 to 0.1875
- mix_gain: float32 [2048], replicated, may hold values from 0.1 to 1.9
- ffn_gain: float32 [2048], replicated, may hold values from 0.1 to 1.9
- out_gain: float32 [2048], replicated, may hold values from 0.1 to 1.9
- gate_weight: bfloat16 [2048, 5120], P('sp', 'tp'), may hold values from -0.125 to 0.125
- up_weight: bfloat16 [2048, 5120], P('sp', 'tp'), may hold values from -0.125 to 0.125
- down_weight: bfloat16 [2048, 5120], P('sp', 'tp'), may hold values from -0.078125 to 0.078125
Outputs:
- layer_out: bfloat16 [1024, 2048], P(('grp', 'sp')), parts along dimension 0
The draws below stay inside these ranges and needn't reach their ends.
There are 2 independent parts, one for each index of `grp`. The reference program is written for one: setup_inputs(seed, part) draws one part's arguments, and reference() takes and returns one part's arrays. A program takes and returns all parts, laid end to end along the dimension named above; an argument that names none is the same for every part. Nothing has to cross between parts.
Inputs may be any that keep to these rules, and one draw needn't show every extreme that they name: `key_logit`: log-odds offsets of the keys, all negative.
All inputs are finite; a program needn't handle non-finite values.
Results may differ from the reference program's by a relative error of at most 0.018.
Values may be sent and summed in bfloat16 or wider, within the bound.
A program may use at most 64 MiB of HBM per device.

```python
import math
import jax
import jax.numpy as jnp
from jax import lax

D = 2048
ATTENTION_COUNT = 8
HEAD_DIM = 128
FF = 5120
TOK_DEV = 128
SEQUENCE_LENGTH = 512
HEAD_GROUP = 2
FF_GROUP = 1280
N_SP = 4
N_TP = 4


def draw_key_logit(key, part):
    flowing_entries = jax.random.split(key, 5)
    length_log = math.log(SEQUENCE_LENGTH)
    starting_shift = jax.random.uniform(flowing_entries[0], (ATTENTION_COUNT,), jnp.float32, -7.5 - length_log, -8.5)
    tile_spacing = jax.random.uniform(flowing_entries[1], (SEQUENCE_LENGTH // TOK_DEV, ATTENTION_COUNT), jnp.float32, -0.7, 0.7)
    tile_spacing = jnp.repeat(tile_spacing, TOK_DEV, axis=0)
    gaussian_perturbation = 0.3 * jax.random.normal(flowing_entries[2], (SEQUENCE_LENGTH, ATTENTION_COUNT), jnp.float32)
    spots = jax.random.randint(flowing_entries[3], (3, ATTENTION_COUNT), 0, SEQUENCE_LENGTH)
    places = jnp.arange(SEQUENCE_LENGTH, dtype=jnp.int32)[:, None, None]
    hit_entries = jnp.any(places == spots[None, :, :], axis=1)
    sudden_entries = jax.random.uniform(flowing_entries[4], (SEQUENCE_LENGTH, ATTENTION_COUNT), jnp.float32, -1.5, -0.5)
    payload_table = jnp.where(hit_entries, sudden_entries, starting_shift[None, :] + tile_spacing + gaussian_perturbation)
    return payload_table.astype(jnp.bfloat16)


def levels(own_key, shape, cuts, low, top_value):
    level, own = 1.0, jax.random.fold_in(own_key, 6)
    for dim, shards_of in cuts:
        draws = jnp.exp(jax.random.uniform(jax.random.fold_in(own, dim), (shards_of,), jnp.float32, low / len(cuts), top_value / len(cuts)))
        level = level * jnp.repeat(draws, shape[dim] // shards_of).reshape([-1 if axis == dim else 1 for axis in range(len(shape))])
    return level


def normal_values(key, dims, spread, reach, cuts=(), kind=jnp.bfloat16):
    array = spread * jax.random.normal(key, dims, jnp.float32)
    if cuts:
        array = array * levels(key, dims, cuts, -0.22, 0.18)
    return jnp.clip(array, -reach, reach).astype(kind)


def setup_inputs(seed: int = 0, part: int = 0) -> dict:
    key_list = jax.random.split(jax.random.key(seed), 13)
    part_keys = jax.random.split(jax.random.fold_in(key_list[12], part), 13)
    return {
        "query_rows": normal_values(part_keys[0], (SEQUENCE_LENGTH, ATTENTION_COUNT * HEAD_DIM), 2.0, 12.0, ((0, 4), (1, 4))),
        "key_rows": normal_values(part_keys[1], (SEQUENCE_LENGTH, ATTENTION_COUNT * HEAD_DIM), 1.5, 9.0, ((0, 4), (1, 4))),
        "value_rows": normal_values(part_keys[2], (SEQUENCE_LENGTH, ATTENTION_COUNT * HEAD_DIM), 1.0, 6.0, ((0, 4), (1, 4))),
        "key_logit": draw_key_logit(jax.random.fold_in(jax.random.fold_in(key_list[12], part), 71), part),
        "residual": normal_values(part_keys[4], (SEQUENCE_LENGTH, D), 1.0, 6.0, ((0, 4),)),
        "out_weight": normal_values(key_list[5], (ATTENTION_COUNT * HEAD_DIM, D), (ATTENTION_COUNT * HEAD_DIM) ** -0.5, 0.1875, ((0, 4),)),
        "mix_gain": jnp.clip(1.0 + 0.18 * jax.random.normal(key_list[6], (D,), jnp.float32), 0.1, 1.9),
        "ffn_gain": jnp.clip(1.0 + 0.18 * jax.random.normal(key_list[7], (D,), jnp.float32), 0.1, 1.9),
        "out_gain": jnp.clip(1.0 + 0.18 * jax.random.normal(key_list[8], (D,), jnp.float32), 0.1, 1.9),
        "gate_weight": normal_values(key_list[9], (D, FF), D ** -0.5, 0.125, ((0, 4), (1, 4))),
        "up_weight": normal_values(key_list[10], (D, FF), D ** -0.5, 0.125, ((0, 4), (1, 4))),
        "down_weight": normal_values(key_list[11], (D, FF), FF ** -0.5, 0.078125, ((0, 4), (1, 4))),
    }


epsilon = 1e-06

def normalize(payload_table):
    return payload_table * lax.rsqrt(lax.optimization_barrier(jnp.mean(payload_table * payload_table, axis=-1, keepdims=True)) + epsilon)

def block_terms(queries, key_part, value_part, logit_part, query_block, key_block):
    scores = jnp.einsum('hqd,khd->hqk', queries.astype(jnp.float32), key_part.astype(jnp.float32)) * HEAD_DIM ** (-0.5)
    scores = scores + jnp.transpose(logit_part.astype(jnp.float32))[:, None, :]
    query_pos = query_block * TOK_DEV + jnp.arange(TOK_DEV, dtype=jnp.int32)[:, None]
    key_pos = key_block * TOK_DEV + jnp.arange(TOK_DEV, dtype=jnp.int32)[None, :]
    causal = key_pos < query_pos
    keep_log = jnp.where(causal, jax.nn.log_sigmoid(-scores), 0.0)
    totals = lax.optimization_barrier(jnp.sum(keep_log, axis=2))
    within = lax.cumsum(keep_log, axis=2, reverse=True) - keep_log
    sticks = jnp.where(causal, jnp.exp(jax.nn.log_sigmoid(scores) + within), 0.0).astype(jnp.bfloat16)
    partials = jnp.einsum('hqk,khd->hqd', sticks.astype(jnp.float32), value_part.astype(jnp.float32))
    return (totals, partials)

def reference(query_rows, key_rows, value_rows, key_logit, residual, out_weight, mix_gain, ffn_gain, out_gain, gate_weight, up_weight, down_weight):

    def one_block(query_block):
        start = (query_block * TOK_DEV).astype(jnp.int32)
        queries = lax.dynamic_slice_in_dim(query_rows, start, TOK_DEV, 0).reshape(TOK_DEV, ATTENTION_COUNT, HEAD_DIM).transpose(1, 0, 2)

        def key_terms(key_block):
            key_start = (key_block * TOK_DEV).astype(jnp.int32)
            key_part = lax.dynamic_slice_in_dim(key_rows, key_start, TOK_DEV, 0).reshape(TOK_DEV, ATTENTION_COUNT, HEAD_DIM)
            value_part = lax.dynamic_slice_in_dim(value_rows, key_start, TOK_DEV, 0).reshape(TOK_DEV, ATTENTION_COUNT, HEAD_DIM)
            logit_part = lax.dynamic_slice_in_dim(key_logit, key_start, TOK_DEV, 0)

            def compute(unused):
                return block_terms(queries, key_part, value_part, logit_part, query_block, key_block)

            def skipped(unused):
                return (jnp.zeros((ATTENTION_COUNT, TOK_DEV), jnp.float32), jnp.zeros((ATTENTION_COUNT, TOK_DEV, HEAD_DIM), jnp.float32))
            return lax.cond(key_block <= query_block, compute, skipped, 0)
        totals, partials = lax.map(key_terms, jnp.arange(N_SP, dtype=jnp.int32))
        suffix = lax.cumsum(totals, axis=0, reverse=True) - totals
        attended = jnp.einsum('bhq,bhqd->qhd', jnp.exp(suffix), partials, precision=lax.Precision.HIGHEST)
        attended = attended.reshape(TOK_DEV, ATTENTION_COUNT * HEAD_DIM).astype(jnp.bfloat16)
        head_part = jnp.einsum('qgc,gcd->gqd', attended.reshape(TOK_DEV, N_TP, HEAD_GROUP * HEAD_DIM).astype(jnp.float32), out_weight.reshape(N_TP, HEAD_GROUP * HEAD_DIM, D).astype(jnp.float32)).astype(jnp.bfloat16)
        mixed_rows = lax.optimization_barrier(jnp.sum(head_part.astype(jnp.float32), axis=0)).astype(jnp.bfloat16)
        own_residual = lax.dynamic_slice_in_dim(residual, start, TOK_DEV, 0).astype(jnp.float32)
        middle = (own_residual + mix_gain * normalize(mixed_rows.astype(jnp.float32))).astype(jnp.bfloat16)
        normed = (ffn_gain * normalize(middle.astype(jnp.float32))).astype(jnp.bfloat16)
        gate_act = jnp.dot(normed, gate_weight, preferred_element_type=jnp.float32)
        up_act = jnp.dot(normed, up_weight, preferred_element_type=jnp.float32)
        hidden = (jax.nn.silu(gate_act) * up_act).astype(jnp.bfloat16)
        unit_part = jnp.einsum('qgf,dgf->gqd', hidden.reshape(TOK_DEV, N_TP, FF_GROUP).astype(jnp.float32), down_weight.reshape(D, N_TP, FF_GROUP).astype(jnp.float32)).astype(jnp.bfloat16)
        ffn_out = lax.optimization_barrier(jnp.sum(unit_part.astype(jnp.float32), axis=0)).astype(jnp.bfloat16)
        return (middle.astype(jnp.float32) + out_gain * normalize(ffn_out.astype(jnp.float32))).astype(jnp.bfloat16)
    blocks_out = lax.map(one_block, jnp.arange(N_SP, dtype=jnp.int32))
    return blocks_out.reshape(SEQUENCE_LENGTH, D)
```

```python
import functools

import jax
import jax.numpy as jnp
from jax import lax
from jax.experimental import pallas as pl
from jax.experimental.pallas import tpu as pltpu
from jax.sharding import PartitionSpec as P

epsilon = 1e-06
MESH = pl.DeviceIdType.MESH
F32 = jnp.float32
BF16 = jnp.bfloat16


def normalize(rows):
    return rows * lax.rsqrt(jnp.mean(rows * rows, axis=-1, keepdims=True) + epsilon)


def each(count, body):
    if count <= 4:
        for i in range(count):
            body(i)
    else:

        def step(i, carry):
            body(i)
            return carry

        lax.fori_loop(0, count, step, 0)


def remote(src, dst, send, recv, axis, peer):
    return pltpu.make_async_remote_copy(
        src_ref=src,
        dst_ref=dst,
        send_sem=send,
        recv_sem=recv,
        device_id={axis: peer},
        device_id_type=MESH,
    )


def nt(a, b):
    return lax.dot_general(a, b, (((1,), (1,)), ((), ())), preferred_element_type=F32)


def kernel(
    S, TP, H,
    q, k, v, lg, mg, fg, og, res, ow, gw, uw, dw,
    out,
    kb, vb, lb, acc, run, owv, gwv, uwv, dwv, resv,
    hs, hr, mid, ns, na, tmp, gs, gr, hall, us, ur, zs, zr, oall,
    loc, kvs, kvr, hss, hrs, n1s, n1r, n2s, n2r, gss, grs, hars, hals, har,
    upss, upr, zss, zrs, oss, ors, outs,
):
    me, tp = lax.axis_index("sp"), lax.axis_index("tp")
    T = q.shape[0]
    hd = q.shape[1] // H
    D = out.shape[1]
    R, C = T // TP, D // S
    right, left = lax.rem(me + 1, S), lax.rem(me + S - 1, S)

    my_rows = pl.ds(pl.multiple_of(tp * R, R), R)
    loads = [
        pltpu.make_async_copy(a, b, loc.at[i])
        for i, (a, b) in enumerate(
            [(ow, owv), (res.at[my_rows], resv), (gw, gwv), (uw, uwv), (dw, dwv)]
        )
    ]
    for c in loads:
        c.start()

    barrier = pltpu.get_barrier_semaphore()
    for f in range(1, S):
        pl.semaphore_signal(barrier, inc=1, device_id={"sp": lax.rem(me + f, S)}, device_id_type=MESH)
    for f in range(1, TP):
        pl.semaphore_signal(barrier, inc=1, device_id={"tp": lax.rem(tp + f, TP)}, device_id_type=MESH)
    pl.semaphore_wait(barrier, S + TP - 2)

    def kv_copies(b, own):
        srcs = (k, v, lg) if own else (kb.at[b], vb.at[b], lb.at[b])
        return [
            remote(src, dst.at[b], kvs.at[b, i], kvr.at[b, i], "sp", right)
            for i, (src, dst) in enumerate(zip(srcs, (kb, vb, lb)))
        ]

    @pl.when(me < S - 1)
    def _():
        for c in kv_copies(me, True):
            c.start()

    rows = lax.broadcasted_iota(jnp.int32, (T, T), 0)
    cols = lax.broadcasted_iota(jnp.int32, (T, T), 1)
    causal = cols < rows
    later = (rows > cols).astype(F32)

    def block(kk, vv, ll, diag):
        for h in range(H):
            span = slice(h * hd, (h + 1) * hd)
            s = nt(q[:, span], kk[:, span]) * (hd**-0.5) + ll[h : h + 1, :]
            soft = jnp.log1p(jnp.exp(-jnp.abs(s)))
            keep = jnp.minimum(-s, 0.0) - soft
            logsig = jnp.minimum(s, 0.0) - soft
            if diag:
                keep = jnp.where(causal, keep, 0.0)
            within = jnp.dot(
                keep, later, preferred_element_type=F32, precision=lax.Precision.HIGHEST
            )
            stick = jnp.exp(logsig + within)
            if diag:
                stick = jnp.where(causal, stick, 0.0)
            part = jnp.dot(stick.astype(BF16), vv[:, span], preferred_element_type=F32)
            total = jnp.broadcast_to(jnp.sum(keep, axis=-1, keepdims=True), (T, hd))
            if diag:
                acc[h] = part
                run[h] = total
            else:
                acc[h] += jnp.exp(run[h]) * part
                run[h] += total

    block(k[...], v[...], lg[...], True)

    def earlier(i):
        b = me - 1 - i

        @pl.when(b >= 0)
        def _():
            for c in kv_copies(b, False):
                c.wait_recv()

            @pl.when(me < S - 1)
            def _():
                for c in kv_copies(b, False):
                    c.start()

            block(kb[b], vb[b], lb[b], False)

    each(S - 1, earlier)

    attended = jnp.concatenate([acc[h] for h in range(H)], axis=1).astype(BF16)
    loads[0].wait()
    width = 512 if D % 512 == 0 else D
    for c0 in range(0, D, width):
        piece = jnp.dot(attended, owv[:, c0 : c0 + width], preferred_element_type=F32)
        hs[:, :, c0 : c0 + width] = piece.astype(BF16).reshape(TP, R, width)

    def hp_copy(t, slot):
        return remote(hs.at[t], hr.at[slot], hss.at[t], hrs.at[slot], "tp", t)

    def others(count, own, body):
        def go(i):
            body(lax.rem(own + 1 + i, count))

        each(count - 1, go)

    others(TP, tp, lambda t: hp_copy(t, tp).start())
    mid[...] = hs[tp].astype(F32)

    def add_hp(t):
        hp_copy(t, t).wait_recv()
        mid[...] += hr[t].astype(F32)

    others(TP, tp, add_hp)
    loads[1].wait()
    mixed = mid[...].astype(BF16).astype(F32)
    middle = (resv[...].astype(F32) + mg[...] * normalize(mixed)).astype(BF16).astype(F32)
    mid[...] = middle
    normed = (fg[...] * normalize(middle)).astype(BF16)
    for j in range(S):
        ns[j] = normed[:, j * C : (j + 1) * C]

    def n1_copy(j, slot):
        return remote(ns.at[j], na.at[tp, slot], n1s.at[j], n1r.at[slot], "sp", j)

    def n2_copy(t, slot, s):
        return remote(na.at[tp, s], na.at[slot, s], n2s.at[t, s], n2r.at[slot, s], "tp", t)

    others(S, me, lambda j: n1_copy(j, me).start())
    na[tp, me] = ns[me]
    others(TP, tp, lambda t: n2_copy(t, tp, me).start())

    def pass_on(s):
        n1_copy(s, s).wait_recv()
        others(TP, tp, lambda t: n2_copy(t, tp, s).start())

    others(S, me, pass_on)
    for c in loads[2:4]:
        c.wait()

    def arrive(s):
        others(TP, tp, lambda t: remote(na.at[tp, s], na.at[t, s], n2s.at[t, s], n2r.at[t, s], "tp", t).wait_recv())

    def partial(j):
        arrive(j)
        x = na[:, j].reshape(T, C)
        tmp[0] = jnp.dot(x, gwv[...], preferred_element_type=F32)
        tmp[1] = jnp.dot(x, uwv[...], preferred_element_type=F32)

    def g_copy(j, slot, i, peer):
        return remote(gs.at[j, i], gr.at[slot, i], gss.at[j, i], grs.at[slot, i], "sp", peer)

    def chain(j, first, slot, peer):
        partial(j)

        @pl.when(first)
        def _():
            for i in range(2):
                gs[j, i] = tmp[i].astype(BF16)
                g_copy(j, slot, i, peer).start()

        @pl.when(jnp.logical_not(first))
        def _():
            for i in range(2):
                g_copy(j, j, i, peer).wait_recv()
                gs[j, i] = (tmp[i] + gr[j, i].astype(F32)).astype(BF16)
                g_copy(j, slot, i, peer).start()

    def reduce_step(tau, carry):
        jr = S - 1 - tau + me
        jl = tau - (S - 1 - me)

        @pl.when((jr > me) & (jr < S))
        def _():
            chain(jr, me == 0, jr, right)

        @pl.when((jl >= 0) & (jl < me))
        def _():
            chain(jl, me == S - 1, lax.select(jl == me - 1, S, jl), left)

        return carry

    lax.fori_loop(0, S - 1, reduce_step, 0)
    partial(me)
    for i in range(2):

        @pl.when(me > 0)
        def _():
            g_copy(me, me, i, left).wait_recv()
            tmp[i] += gr[me, i].astype(F32)

        @pl.when(me < S - 1)
        def _():
            g_copy(me, S, i, right).wait_recv()
            tmp[i] += gr[S, i].astype(F32)

    gate = tmp[0]
    hall[me] = (gate / (1.0 + jnp.exp(-gate)) * tmp[1]).astype(BF16)

    def h_right(b):
        return remote(hall.at[b], hall.at[b], hars.at[b], har.at[b], "sp", right)

    def h_left(b):
        return remote(hall.at[b], hall.at[b], hals.at[b], har.at[b], "sp", left)

    @pl.when(me < S - 1)
    def _():
        h_right(me).start()

    @pl.when(me > 0)
    def _():
        h_left(me).start()

    def up_copy(t, slot, b):
        return remote(us.at[t, b], ur.at[slot, b], upss.at[t, b], upr.at[slot, b], "tp", t)

    def down(b):
        us[:, b] = nt(hall[b], dwv[...]).astype(BF16).reshape(TP, R, C)
        others(TP, tp, lambda t: up_copy(t, tp, b).start())

    def z_copy(b, slot):
        return remote(zs.at[b], zr.at[slot], zss.at[b], zrs.at[slot], "sp", b)

    def settle(b):
        total = us[tp, b].astype(F32)
        mid2 = [total]

        def add(t):
            up_copy(t, t, b).wait_recv()
            zs_sum[...] += ur[t, b].astype(F32)

        zs_sum = tmp.at[0, pl.ds(0, R), pl.ds(0, C)]
        zs_sum[...] = mid2[0]
        others(TP, tp, add)
        zs[b] = zs_sum[...].astype(BF16)

        @pl.when(b != me)
        def _():
            z_copy(b, me).start()

    loads[4].wait()
    down(me)

    def spread(i, carry):
        lo, hi = me - 1 - i, me + 1 + i

        @pl.when(lo >= 0)
        def _():
            h_right(lo).wait_recv()

            @pl.when(me < S - 1)
            def _():
                h_right(lo).start()

            down(lo)

        @pl.when(hi < S)
        def _():
            h_left(hi).wait_recv()

            @pl.when(me > 0)
            def _():
                h_left(hi).start()

            down(hi)

        return carry

    lax.fori_loop(0, S - 1, spread, 0)
    others(S, me, settle)
    settle(me)
    zr[me] = zs[me]
    others(S, me, lambda s: z_copy(s, s).wait_recv())
    ffn = jnp.concatenate([zr[s] for s in range(S)], axis=1).astype(F32)
    oall[tp] = (mid[...] + og[...] * normalize(ffn)).astype(BF16)

    def o_copy(t, slot):
        return remote(oall.at[tp], oall.at[slot], oss.at[t], ors.at[slot], "tp", t)

    def o_out(t):
        return pltpu.make_async_copy(
            oall.at[t], out.at[pl.ds(pl.multiple_of(t * R, R), R)], outs.at[t]
        )

    others(TP, tp, lambda t: o_copy(t, tp).start())
    o_out(tp).start()

    def o_in(t):
        remote(oall.at[tp], oall.at[t], oss.at[t], ors.at[t], "tp", t).wait_recv()
        o_out(t).start()

    others(TP, tp, o_in)
    each(TP, lambda t: o_out(t).wait())

    @pl.when(me < S - 1)
    def _():
        def sent(b):
            @pl.when(b <= me)
            def _():
                for c in kv_copies(b, False):
                    c.wait_send()
                h_right(b).wait_send()

        each(S, sent)

    @pl.when(me > 0)
    def _():
        def sent(b):
            @pl.when(b >= me)
            def _():
                h_left(b).wait_send()

        each(S, sent)

    def sp_sent(j):
        n1_copy(j, me).wait_send()
        z_copy(j, me).wait_send()
        for i in range(2):
            g_copy(j, j, i, right).wait_send()

    others(S, me, sp_sent)

    def tp_sent(t):
        hp_copy(t, tp).wait_send()
        o_copy(t, tp).wait_send()

        def inner(s):
            n2_copy(t, tp, s).wait_send()
            up_copy(t, tp, s).wait_send()

        each(S, inner)

    others(TP, tp, tp_sent)


def solution(mesh):
    S, TP = mesh.shape["sp"], mesh.shape["tp"]

    def shards(q, k, v, lg, res, ow, mg, fg, og, gw, uw, dw):
        T, H = lg.shape
        hw = q.shape[1]
        D = res.shape[1]
        C, U = gw.shape
        R = T // TP
        pad = -H % 8
        lgt = jnp.pad(lg.astype(F32).T, ((0, pad), (0, 0)))
        vm = pl.BlockSpec(memory_space=pltpu.VMEM)
        hb = pl.BlockSpec(memory_space=pl.ANY)
        dma = pltpu.SemaphoreType.DMA
        return pl.pallas_call(
            functools.partial(kernel, S, TP, H),
            out_shape=jax.ShapeDtypeStruct((T, D), BF16),
            in_specs=[vm] * 7 + [hb] * 5,
            out_specs=hb,
            scratch_shapes=[
                pltpu.VMEM((S, T, hw), BF16),
                pltpu.VMEM((S, T, hw), BF16),
                pltpu.VMEM((S,) + lgt.shape, F32),
                pltpu.VMEM((H, T, hw // H), F32),
                pltpu.VMEM((H, T, hw // H), F32),
                pltpu.VMEM(ow.shape, BF16),
                pltpu.VMEM(gw.shape, BF16),
                pltpu.VMEM(uw.shape, BF16),
                pltpu.VMEM(dw.shape, BF16),
                pltpu.VMEM((R, D), BF16),
                pltpu.VMEM((TP, R, D), BF16),
                pltpu.VMEM((TP, R, D), BF16),
                pltpu.VMEM((R, D), F32),
                pltpu.VMEM((S, R, C), BF16),
                pltpu.VMEM((TP, S, R, C), BF16),
                pltpu.VMEM((2, T, U), F32),
                pltpu.VMEM((S, 2, T, U), BF16),
                pltpu.VMEM((S + 1, 2, T, U), BF16),
                pltpu.VMEM((S, T, U), BF16),
                pltpu.VMEM((TP, S, R, C), BF16),
                pltpu.VMEM((TP, S, R, C), BF16),
                pltpu.VMEM((S, R, C), BF16),
                pltpu.VMEM((S, R, C), BF16),
                pltpu.VMEM((TP, R, D), BF16),
                dma((5,)),
                dma((S, 3)),
                dma((S, 3)),
                dma((TP,)),
                dma((TP,)),
                dma((S,)),
                dma((S,)),
                dma((TP, S)),
                dma((TP, S)),
                dma((S, 2)),
                dma((S + 1, 2)),
                dma((S,)),
                dma((S,)),
                dma((S,)),
                dma((TP, S)),
                dma((TP, S)),
                dma((S,)),
                dma((S,)),
                dma((TP,)),
                dma((TP,)),
                dma((TP,)),
            ],
            compiler_params=pltpu.CompilerParams(
                collective_id=0, has_side_effects=True, vmem_limit_bytes=67043328 - 2**20
            ),
        )(q, k, v, lgt, mg[None], fg[None], og[None], res, ow, gw, uw, dw)

    placed = (
        P(("grp", "sp"), "tp"),
        P(("grp", "sp"), "tp"),
        P(("grp", "sp"), "tp"),
        P(("grp", "sp"), "tp"),
        P(("grp", "sp"), None),
        P("tp", None),
        P(),
        P(),
        P(),
        P("sp", "tp"),
        P("sp", "tp"),
        P("sp", "tp"),
    )
    return jax.shard_map(
        shards, mesh=mesh, in_specs=placed, out_specs=P(("grp", "sp"), None), check_vma=False
    )
```

```python
import functools

import jax
import jax.numpy as jnp
from jax import lax
from jax.experimental import pallas as pl
from jax.experimental.pallas import tpu as pltpu
from jax.sharding import PartitionSpec as P

epsilon = 1e-06
MESH = pl.DeviceIdType.MESH
F32 = jnp.float32
BF16 = jnp.bfloat16


def normalize(rows):
    return rows * lax.rsqrt(jnp.mean(rows * rows, axis=-1, keepdims=True) + epsilon)


def each(count, body):
    if count <= 4:
        for i in range(count):
            body(i)
    else:

        def step(i, carry):
            body(i)
            return carry

        lax.fori_loop(0, count, step, 0)


def remote(src, dst, send, recv, axis, peer):
    return pltpu.make_async_remote_copy(
        src_ref=src,
        dst_ref=dst,
        send_sem=send,
        recv_sem=recv,
        device_id={axis: peer},
        device_id_type=MESH,
    )


def nt(a, b):
    return lax.dot_general(a, b, (((1,), (1,)), ((), ())), preferred_element_type=F32)


def kernel(
    S, TP, H, pieces,
    q, k, v, lg, mg, fg, og, res, ow, gw, uw, dw,
    out,
    kb, vb, lb, acc, run, owv, gwv, uwv, dwv, resv,
    hs, hr, mid, zs_sum, ns, na, tmp, gs, gr, hall, us, ur, zs, zr, oall,
    loc, kvs, kvr, hss, hrs, n1s, n1r, n2s, n2r, gss, grs, hars, hals, har,
    upss, upr, zss, zrs, oss, ors, outs,
):
    me, tp = lax.axis_index("sp"), lax.axis_index("tp")
    T = q.shape[0]
    hd = q.shape[1] // H
    D = out.shape[1]
    R, C = T // TP, D // S
    right, left = lax.rem(me + 1, S), lax.rem(me + S - 1, S)

    my_rows = pl.ds(pl.multiple_of(tp * R, R), R)
    loads = [
        pltpu.make_async_copy(a, b, loc.at[i])
        for i, (a, b) in enumerate(
            [(ow, owv), (res.at[my_rows], resv), (gw, gwv), (uw, uwv), (dw, dwv)]
        )
    ]
    for c in loads:
        c.start()

    barrier = pltpu.get_barrier_semaphore()
    for f in range(1, S):
        pl.semaphore_signal(barrier, inc=1, device_id={"sp": lax.rem(me + f, S)}, device_id_type=MESH)
    for f in range(1, TP):
        pl.semaphore_signal(barrier, inc=1, device_id={"tp": lax.rem(tp + f, TP)}, device_id_type=MESH)
    pl.semaphore_wait(barrier, S + TP - 2)

    def kv_copies(b, own):
        srcs = (k, v, lg) if own else (kb.at[b], vb.at[b], lb.at[b])
        return [
            remote(src, dst.at[b], kvs.at[b, i], kvr.at[b, i], "sp", right)
            for i, (src, dst) in enumerate(zip(srcs, (kb, vb, lb)))
        ]

    @pl.when(me < S - 1)
    def _():
        for c in kv_copies(me, True):
            c.start()

    rows = lax.broadcasted_iota(jnp.int32, (T, T), 0)
    cols = lax.broadcasted_iota(jnp.int32, (T, T), 1)
    causal = cols < rows
    later = (rows > cols).astype(F32)

    def block(kk, vv, ll, diag):
        for h in range(H):
            span = slice(h * hd, (h + 1) * hd)
            s = nt(q[:, span], kk[:, span]) * (hd**-0.5) + ll[h : h + 1, :]
            soft = jnp.log1p(jnp.exp(-jnp.abs(s)))
            keep = jnp.minimum(-s, 0.0) - soft
            logsig = jnp.minimum(s, 0.0) - soft
            if diag:
                keep = jnp.where(causal, keep, 0.0)
            within = jnp.dot(
                keep, later, preferred_element_type=F32, precision=lax.Precision.HIGHEST
            )
            stick = jnp.exp(logsig + within)
            if diag:
                stick = jnp.where(causal, stick, 0.0)
            part = jnp.dot(stick.astype(BF16), vv[:, span], preferred_element_type=F32)
            total = jnp.broadcast_to(jnp.sum(keep, axis=-1, keepdims=True), (T, hd))
            if diag:
                acc[h] = part
                run[h] = total
            else:
                acc[h] += jnp.exp(run[h]) * part
                run[h] += total

    block(k[...], v[...], lg[...], True)

    def earlier(i):
        b = me - 1 - i

        @pl.when(b >= 0)
        def _():
            for c in kv_copies(b, False):
                c.wait_recv()

            @pl.when(me < S - 1)
            def _():
                for c in kv_copies(b, False):
                    c.start()

            block(kb[b], vb[b], lb[b], False)

    each(S - 1, earlier)

    attended = jnp.concatenate([acc[h] for h in range(H)], axis=1).astype(BF16)
    loads[0].wait()
    width = 512 if D % 512 == 0 else D
    for c0 in range(0, D, width):
        piece = jnp.dot(attended, owv[:, c0 : c0 + width], preferred_element_type=F32)
        hs[:, :, c0 : c0 + width] = piece.astype(BF16).reshape(TP, R, width)

    def hp_copy(t, slot):
        return remote(hs.at[t], hr.at[slot], hss.at[t], hrs.at[slot], "tp", t)

    def others(count, own, body):
        def go(i):
            body(lax.rem(own + 1 + i, count))

        each(count - 1, go)

    others(TP, tp, lambda t: hp_copy(t, tp).start())
    mid[...] = hs[tp].astype(F32)

    def add_hp(t):
        hp_copy(t, t).wait_recv()
        mid[...] += hr[t].astype(F32)

    others(TP, tp, add_hp)
    loads[1].wait()
    mixed = mid[...].astype(BF16).astype(F32)
    middle = (resv[...].astype(F32) + mg[...] * normalize(mixed)).astype(BF16).astype(F32)
    mid[...] = middle
    normed = (fg[...] * normalize(middle)).astype(BF16)
    for j in range(S):
        ns[j] = normed[:, j * C : (j + 1) * C]

    def n1_copy(j, slot):
        return remote(ns.at[j], na.at[tp, slot], n1s.at[j], n1r.at[slot], "sp", j)

    def n2_copy(t, slot, s):
        return remote(na.at[tp, s], na.at[slot, s], n2s.at[t, s], n2r.at[slot, s], "tp", t)

    others(S, me, lambda j: n1_copy(j, me).start())
    na[tp, me] = ns[me]
    others(TP, tp, lambda t: n2_copy(t, tp, me).start())

    def pass_on(s):
        n1_copy(s, s).wait_recv()
        others(TP, tp, lambda t: n2_copy(t, tp, s).start())

    others(S, me, pass_on)
    for c in loads[2:4]:
        c.wait()

    def arrive(s):
        others(TP, tp, lambda t: remote(na.at[tp, s], na.at[t, s], n2s.at[t, s], n2r.at[t, s], "tp", t).wait_recv())

    W = gs.shape[-1]

    def partial(p, j):
        @pl.when(p == 0)
        def _():
            arrive(j)

        x = na[:, j].reshape(T, C)
        units = pl.ds(pl.multiple_of(p * W, W), W)
        tmp[0] = jnp.dot(x, gwv[:, units], preferred_element_type=F32)
        tmp[1] = jnp.dot(x, uwv[:, units], preferred_element_type=F32)

    def g_copy(p, j, slot, peer):
        return remote(gs.at[p, j], gr.at[p, slot], gss.at[p, j], grs.at[p, slot], "sp", peer)

    def chain(p, j, first, slot, peer):
        partial(p, j)

        @pl.when(first)
        def _():
            gs[p, j] = tmp[...].astype(BF16)

        @pl.when(jnp.logical_not(first))
        def _():
            g_copy(p, j, j, peer).wait_recv()
            gs[p, j] = (tmp[...] + gr[p, j].astype(F32)).astype(BF16)

        g_copy(p, j, slot, peer).start()

    def h_right(p, b):
        return remote(hall.at[p, b], hall.at[p, b], hars.at[p, b], har.at[p, b], "sp", right)

    def h_left(p, b):
        return remote(hall.at[p, b], hall.at[p, b], hals.at[p, b], har.at[p, b], "sp", left)

    def reduce_step(p, tau):
        jr = S - 1 - tau + me
        jl = tau - (S - 1 - me)

        @pl.when((jr > me) & (jr < S))
        def _():
            chain(p, jr, me == 0, jr, right)

        @pl.when((jl >= 0) & (jl < me))
        def _():
            chain(p, jl, me == S - 1, lax.select(jl == me - 1, S, jl), left)

    def finish(p):
        partial(p, me)

        @pl.when(me > 0)
        def _():
            g_copy(p, me, me, left).wait_recv()
            tmp[...] += gr[p, me].astype(F32)

        @pl.when(me < S - 1)
        def _():
            g_copy(p, me, S, right).wait_recv()
            tmp[...] += gr[p, S].astype(F32)

        gate = tmp[0]
        hall[p, me] = (gate / (1.0 + jnp.exp(-gate)) * tmp[1]).astype(BF16)

        @pl.when(me < S - 1)
        def _():
            h_right(p, me).start()

        @pl.when(me > 0)
        def _():
            h_left(p, me).start()

    def spread(p, i, then):
        lo, hi = me - 1 - i, me + 1 + i

        @pl.when(lo >= 0)
        def _():
            h_right(p, lo).wait_recv()

            @pl.when(me < S - 1)
            def _():
                h_right(p, lo).start()

            then(lo)

        @pl.when(hi < S)
        def _():
            h_left(p, hi).wait_recv()

            @pl.when(me > 0)
            def _():
                h_left(p, hi).start()

            then(hi)

    def step(g, carry):
        p, tau = g // (S - 1), lax.rem(g, S - 1)

        @pl.when(p < pieces)
        def _():
            reduce_step(p, tau)

        @pl.when((tau == 0) & (p >= 1))
        def _():
            finish(p - 1)

        @pl.when(p >= 2)
        def _():
            spread(p - 2, tau, lambda b: None)

        return carry

    lax.fori_loop(0, (pieces + 1) * (S - 1), step, 0)

    def up_copy(t, slot, b):
        return remote(us.at[t, b], ur.at[slot, b], upss.at[t, b], upr.at[slot, b], "tp", t)

    def down(b):
        rows_b = jnp.concatenate([hall[p, b] for p in range(pieces)], axis=1)
        us[:, b] = nt(rows_b, dwv[...]).astype(BF16).reshape(TP, R, C)
        others(TP, tp, lambda t: up_copy(t, tp, b).start())

    def z_copy(b, slot):
        return remote(zs.at[b], zr.at[slot], zss.at[b], zrs.at[slot], "sp", b)

    def settle(b):
        def add(t):
            up_copy(t, t, b).wait_recv()
            zs_sum[...] += ur[t, b].astype(F32)

        zs_sum[...] = us[tp, b].astype(F32)
        others(TP, tp, add)
        zs[b] = zs_sum[...].astype(BF16)

        @pl.when(b != me)
        def _():
            z_copy(b, me).start()

    loads[4].wait()
    down(me)

    def last(i, carry):
        spread(pieces - 1, i, down)
        return carry

    lax.fori_loop(0, S - 1, last, 0)
    others(S, me, settle)
    settle(me)
    zr[me] = zs[me]
    others(S, me, lambda s: z_copy(s, s).wait_recv())
    ffn = jnp.concatenate([zr[s] for s in range(S)], axis=1).astype(F32)
    oall[tp] = (mid[...] + og[...] * normalize(ffn)).astype(BF16)

    def o_copy(t, slot):
        return remote(oall.at[tp], oall.at[slot], oss.at[t], ors.at[slot], "tp", t)

    def o_out(t):
        return pltpu.make_async_copy(
            oall.at[t], out.at[pl.ds(pl.multiple_of(t * R, R), R)], outs.at[t]
        )

    others(TP, tp, lambda t: o_copy(t, tp).start())
    o_out(tp).start()

    def o_in(t):
        remote(oall.at[tp], oall.at[t], oss.at[t], ors.at[t], "tp", t).wait_recv()
        o_out(t).start()

    others(TP, tp, o_in)
    each(TP, lambda t: o_out(t).wait())

    @pl.when(me < S - 1)
    def _():
        def sent(b):
            @pl.when(b <= me)
            def _():
                for c in kv_copies(b, False):
                    c.wait_send()
                each(pieces, lambda p: h_right(p, b).wait_send())

        each(S, sent)

    @pl.when(me > 0)
    def _():
        def sent(b):
            @pl.when(b >= me)
            def _():
                each(pieces, lambda p: h_left(p, b).wait_send())

        each(S, sent)

    def sp_sent(j):
        n1_copy(j, me).wait_send()
        z_copy(j, me).wait_send()
        each(pieces, lambda p: g_copy(p, j, j, right).wait_send())

    others(S, me, sp_sent)

    def tp_sent(t):
        hp_copy(t, tp).wait_send()
        o_copy(t, tp).wait_send()

        def inner(s):
            n2_copy(t, tp, s).wait_send()
            up_copy(t, tp, s).wait_send()

        each(S, inner)

    others(TP, tp, tp_sent)


def solution(mesh):
    S, TP = mesh.shape["sp"], mesh.shape["tp"]

    def shards(q, k, v, lg, res, ow, mg, fg, og, gw, uw, dw):
        T, H = lg.shape
        hw = q.shape[1]
        D = res.shape[1]
        C, U = gw.shape
        R = T // TP
        pieces = max([p for p in range(1, 6) if U % (128 * p) == 0], default=1)
        W = U // pieces
        pad = -H % 8
        lgt = jnp.pad(lg.astype(F32).T, ((0, pad), (0, 0)))
        vm = pl.BlockSpec(memory_space=pltpu.VMEM)
        hb = pl.BlockSpec(memory_space=pl.ANY)
        dma = pltpu.SemaphoreType.DMA
        return pl.pallas_call(
            functools.partial(kernel, S, TP, H, pieces),
            out_shape=jax.ShapeDtypeStruct((T, D), BF16),
            in_specs=[vm] * 7 + [hb] * 5,
            out_specs=hb,
            scratch_shapes=[
                pltpu.VMEM((S, T, hw), BF16),
                pltpu.VMEM((S, T, hw), BF16),
                pltpu.VMEM((S,) + lgt.shape, F32),
                pltpu.VMEM((H, T, hw // H), F32),
                pltpu.VMEM((H, T, hw // H), F32),
                pltpu.VMEM(ow.shape, BF16),
                pltpu.VMEM(gw.shape, BF16),
                pltpu.VMEM(uw.shape, BF16),
                pltpu.VMEM(dw.shape, BF16),
                pltpu.VMEM((R, D), BF16),
                pltpu.VMEM((TP, R, D), BF16),
                pltpu.VMEM((TP, R, D), BF16),
                pltpu.VMEM((R, D), F32),
                pltpu.VMEM((R, C), F32),
                pltpu.VMEM((S, R, C), BF16),
                pltpu.VMEM((TP, S, R, C), BF16),
                pltpu.VMEM((2, T, W), F32),
                pltpu.VMEM((pieces, S, 2, T, W), BF16),
                pltpu.VMEM((pieces, S + 1, 2, T, W), BF16),
                pltpu.VMEM((pieces, S, T, W), BF16),
                pltpu.VMEM((TP, S, R, C), BF16),
                pltpu.VMEM((TP, S, R, C), BF16),
                pltpu.VMEM((S, R, C), BF16),
                pltpu.VMEM((S, R, C), BF16),
                pltpu.VMEM((TP, R, D), BF16),
                dma((5,)),
                dma((S, 3)),
                dma((S, 3)),
                dma((TP,)),
                dma((TP,)),
                dma((S,)),
                dma((S,)),
                dma((TP, S)),
                dma((TP, S)),
                dma((pieces, S)),
                dma((pieces, S + 1)),
                dma((pieces, S)),
                dma((pieces, S)),
                dma((pieces, S)),
                dma((TP, S)),
                dma((TP, S)),
                dma((S,)),
                dma((S,)),
                dma((TP,)),
                dma((TP,)),
                dma((TP,)),
            ],
            compiler_params=pltpu.CompilerParams(
                collective_id=0, has_side_effects=True, vmem_limit_bytes=67043328 - 2**20
            ),
        )(q, k, v, lgt, mg[None], fg[None], og[None], res, ow, gw, uw, dw)

    placed = (
        P(("grp", "sp"), "tp"),
        P(("grp", "sp"), "tp"),
        P(("grp", "sp"), "tp"),
        P(("grp", "sp"), "tp"),
        P(("grp", "sp"), None),
        P("tp", None),
        P(),
        P(),
        P(),
        P("sp", "tp"),
        P("sp", "tp"),
        P("sp", "tp"),
    )
    return jax.shard_map(
        shards, mesh=mesh, in_specs=placed, out_specs=P(("grp", "sp"), None), check_vma=False
    )
```

```python
import functools

import jax
import jax.numpy as jnp
from jax import lax
from jax.experimental import pallas as pl
from jax.experimental.pallas import tpu as pltpu
from jax.sharding import PartitionSpec as P

epsilon = 1e-06
MESH = pl.DeviceIdType.MESH
F32 = jnp.float32
BF16 = jnp.bfloat16
LAG = 2
MOST_PIECES = 5


def normalize(rows):
    return rows * lax.rsqrt(jnp.mean(rows * rows, axis=-1, keepdims=True) + epsilon)


def each(count, body):
    if count <= 4:
        for i in range(count):
            body(i)
    else:

        def step(i, carry):
            body(i)
            return carry

        lax.fori_loop(0, count, step, 0)


def remote(src, dst, send, recv, axis, peer):
    return pltpu.make_async_remote_copy(
        src_ref=src,
        dst_ref=dst,
        send_sem=send,
        recv_sem=recv,
        device_id={axis: peer},
        device_id_type=MESH,
    )


def nt(a, b):
    return lax.dot_general(a, b, (((1,), (1,)), ((), ())), preferred_element_type=F32)


def kernel(
    S, TP, H, pieces,
    q, k, v, lg, mg, fg, og, res, ow, gw, uw, dw,
    out,
    kb, vb, lb, acc, run, owv, gwv, uwv, dwv, resv,
    hs, hr, mid, zs_sum, ns, na, tmp, gs, gr, hall, us, ur, zs, zr, oall,
    loc, kvs, kvr, hss, hrs, n1s, n1r, n2s, n2r, gss, grs, hars, hals, har,
    upss, upr, zss, zrs, oss, ors, outs,
):
    me, tp = lax.axis_index("sp"), lax.axis_index("tp")
    T = q.shape[0]
    hd = q.shape[1] // H
    D = out.shape[1]
    R, C = T // TP, D // S
    right, left = lax.rem(me + 1, S), lax.rem(me + S - 1, S)

    my_rows = pl.ds(pl.multiple_of(tp * R, R), R)
    loads = [
        pltpu.make_async_copy(a, b, loc.at[i])
        for i, (a, b) in enumerate(
            [(ow, owv), (res.at[my_rows], resv), (gw, gwv), (uw, uwv), (dw, dwv)]
        )
    ]
    for c in loads:
        c.start()

    barrier = pltpu.get_barrier_semaphore()
    for f in range(1, S):
        pl.semaphore_signal(barrier, inc=1, device_id={"sp": lax.rem(me + f, S)}, device_id_type=MESH)
    for f in range(1, TP):
        pl.semaphore_signal(barrier, inc=1, device_id={"tp": lax.rem(tp + f, TP)}, device_id_type=MESH)
    pl.semaphore_wait(barrier, S + TP - 2)

    def kv_copies(b, own):
        srcs = (k, v, lg) if own else (kb.at[b], vb.at[b], lb.at[b])
        return [
            remote(src, dst.at[b], kvs.at[b, i], kvr.at[b, i], "sp", right)
            for i, (src, dst) in enumerate(zip(srcs, (kb, vb, lb)))
        ]

    @pl.when(me < S - 1)
    def _():
        for c in kv_copies(me, True):
            c.start()

    rows = lax.broadcasted_iota(jnp.int32, (T, T), 0)
    cols = lax.broadcasted_iota(jnp.int32, (T, T), 1)
    causal = cols < rows
    later = (rows > cols).astype(F32)

    def block(kk, vv, ll, diag):
        for h in range(H):
            span = slice(h * hd, (h + 1) * hd)
            s = nt(q[:, span], kk[:, span]) * (hd**-0.5) + ll[h : h + 1, :]
            soft = jnp.log1p(jnp.exp(-jnp.abs(s)))
            keep = jnp.minimum(-s, 0.0) - soft
            logsig = jnp.minimum(s, 0.0) - soft
            if diag:
                keep = jnp.where(causal, keep, 0.0)
            within = jnp.dot(
                keep, later, preferred_element_type=F32, precision=lax.Precision.HIGHEST
            )
            stick = jnp.exp(logsig + within)
            if diag:
                stick = jnp.where(causal, stick, 0.0)
            part = jnp.dot(stick.astype(BF16), vv[:, span], preferred_element_type=F32)
            total = jnp.broadcast_to(jnp.sum(keep, axis=-1, keepdims=True), (T, hd))
            if diag:
                acc[h] = part
                run[h] = total
            else:
                acc[h] += jnp.exp(run[h]) * part
                run[h] += total

    block(k[...], v[...], lg[...], True)

    def earlier(i):
        b = me - 1 - i

        @pl.when(b >= 0)
        def _():
            for c in kv_copies(b, False):
                c.wait_recv()

            @pl.when(me < S - 1)
            def _():
                for c in kv_copies(b, False):
                    c.start()

            block(kb[b], vb[b], lb[b], False)

    each(S - 1, earlier)

    attended = jnp.concatenate([acc[h] for h in range(H)], axis=1).astype(BF16)
    loads[0].wait()
    width = 512 if D % 512 == 0 else D
    for c0 in range(0, D, width):
        piece = jnp.dot(attended, owv[:, c0 : c0 + width], preferred_element_type=F32)
        hs[:, :, c0 : c0 + width] = piece.astype(BF16).reshape(TP, R, width)

    def hp_copy(t, slot):
        return remote(hs.at[t], hr.at[slot], hss.at[t], hrs.at[slot], "tp", t)

    def others(count, own, body):
        def go(i):
            body(lax.rem(own + 1 + i, count))

        each(count - 1, go)

    others(TP, tp, lambda t: hp_copy(t, tp).start())
    mid[...] = hs[tp].astype(F32)

    def add_hp(t):
        hp_copy(t, t).wait_recv()
        mid[...] += hr[t].astype(F32)

    others(TP, tp, add_hp)
    loads[1].wait()
    mixed = mid[...].astype(BF16).astype(F32)
    middle = (resv[...].astype(F32) + mg[...] * normalize(mixed)).astype(BF16).astype(F32)
    mid[...] = middle
    normed = (fg[...] * normalize(middle)).astype(BF16)
    for j in range(S):
        ns[j] = normed[:, j * C : (j + 1) * C]

    def n1_copy(j, slot):
        return remote(ns.at[j], na.at[tp, slot], n1s.at[j], n1r.at[slot], "sp", j)

    def n2_copy(t, slot, s):
        return remote(na.at[tp, s], na.at[slot, s], n2s.at[t, s], n2r.at[slot, s], "tp", t)

    others(S, me, lambda j: n1_copy(j, me).start())
    na[tp, me] = ns[me]
    others(TP, tp, lambda t: n2_copy(t, tp, me).start())

    def pass_on(s):
        n1_copy(s, s).wait_recv()
        others(TP, tp, lambda t: n2_copy(t, tp, s).start())

    others(S, me, pass_on)
    for c in loads[2:4]:
        c.wait()

    def arrive(s):
        others(TP, tp, lambda t: remote(na.at[tp, s], na.at[t, s], n2s.at[t, s], n2r.at[t, s], "tp", t).wait_recv())

    W = gs.shape[-1]
    lag = LAG

    def partial(p, j):
        @pl.when(p == 0)
        def _():
            arrive(j)

        x = na[:, j].reshape(T, C)
        units = pl.ds(pl.multiple_of(p * W, W), W)
        tmp[0] = jnp.dot(x, gwv[:, units], preferred_element_type=F32)
        tmp[1] = jnp.dot(x, uwv[:, units], preferred_element_type=F32)

    def g_copy(p, j, slot, peer):
        return remote(gs.at[p, j], gr.at[p, slot], gss.at[p, j], grs.at[p, slot], "sp", peer)

    def chain(p, j, first, slot, peer):
        partial(p, j)

        @pl.when(first)
        def _():
            gs[p, j] = tmp[...].astype(BF16)

        @pl.when(jnp.logical_not(first))
        def _():
            g_copy(p, j, j, peer).wait_recv()
            gs[p, j] = (tmp[...] + gr[p, j].astype(F32)).astype(BF16)

        g_copy(p, j, slot, peer).start()

    def h_right(p, b):
        return remote(hall.at[p, b], hall.at[p, b], hars.at[p, b], har.at[p, b], "sp", right)

    def h_left(p, b):
        return remote(hall.at[p, b], hall.at[p, b], hals.at[p, b], har.at[p, b], "sp", left)

    def cut(at):
        return lax.div(at, S - 1), lax.rem(at, S - 1)

    def reduce_step(g):
        at_right = g - me * lag
        at_left = g - (S - 1 - me) * lag

        @pl.when((at_right >= 0) & (at_right < pieces * (S - 1)))
        def _():
            p, tau = cut(at_right)

            @pl.when(S - 1 - tau > me)
            def _():
                chain(p, S - 1 - tau, me == 0, S - 1 - tau, right)

        @pl.when((at_left >= 0) & (at_left < pieces * (S - 1)))
        def _():
            p, j = cut(at_left)

            @pl.when(j < me)
            def _():
                chain(p, j, me == S - 1, lax.select(j == me - 1, S, j), left)

    def finish(p):
        partial(p, me)

        @pl.when(me > 0)
        def _():
            g_copy(p, me, me, left).wait_recv()
            tmp[...] += gr[p, me].astype(F32)

        @pl.when(me < S - 1)
        def _():
            g_copy(p, me, S, right).wait_recv()
            tmp[...] += gr[p, S].astype(F32)

        gate = tmp[0]
        hall[p, me] = (gate / (1.0 + jnp.exp(-gate)) * tmp[1]).astype(BF16)

        @pl.when(me < S - 1)
        def _():
            h_right(p, me).start()

        @pl.when(me > 0)
        def _():
            h_left(p, me).start()

    def spread(p, i, then):
        lo, hi = me - 1 - i, me + 1 + i

        @pl.when(lo >= 0)
        def _():
            h_right(p, lo).wait_recv()

            @pl.when(me < S - 1)
            def _():
                h_right(p, lo).start()

            then(lo)

        @pl.when(hi < S)
        def _():
            h_left(p, hi).wait_recv()

            @pl.when(me > 0)
            def _():
                h_left(p, hi).start()

            then(hi)

    def step(g, carry):
        reduce_step(g)
        at = g - (S - 1) * lag
        p, tau = cut(at)

        @pl.when((at >= 0) & (tau == 0) & (p < pieces))
        def _():
            finish(p)

        def gather(i, carry):
            at_i = at - (i + 1) * lag
            p, tau = cut(at_i)

            @pl.when((at_i >= 0) & (tau == 0) & (p < pieces - 1))
            def _():
                spread(p, i, lambda b: None)

            return carry

        return lax.fori_loop(0, S - 1, gather, carry)

    steps = (S - 1) * (lag + max(pieces - 1, pieces - 2 + lag)) + 1
    lax.fori_loop(0, steps, step, 0)

    def up_copy(t, slot, b):
        return remote(us.at[t, b], ur.at[slot, b], upss.at[t, b], upr.at[slot, b], "tp", t)

    def down(b):
        rows_b = jnp.concatenate([hall[p, b] for p in range(pieces)], axis=1)
        us[:, b] = nt(rows_b, dwv[...]).astype(BF16).reshape(TP, R, C)
        others(TP, tp, lambda t: up_copy(t, tp, b).start())

    def z_copy(b, slot):
        return remote(zs.at[b], zr.at[slot], zss.at[b], zrs.at[slot], "sp", b)

    def settle(b):
        def add(t):
            up_copy(t, t, b).wait_recv()
            zs_sum[...] += ur[t, b].astype(F32)

        zs_sum[...] = us[tp, b].astype(F32)
        others(TP, tp, add)
        zs[b] = zs_sum[...].astype(BF16)

        @pl.when(b != me)
        def _():
            z_copy(b, me).start()

    loads[4].wait()
    down(me)

    def last(i, carry):
        spread(pieces - 1, i, down)
        return carry

    lax.fori_loop(0, S - 1, last, 0)
    others(S, me, settle)
    settle(me)
    zr[me] = zs[me]
    others(S, me, lambda s: z_copy(s, s).wait_recv())
    ffn = jnp.concatenate([zr[s] for s in range(S)], axis=1).astype(F32)
    oall[tp] = (mid[...] + og[...] * normalize(ffn)).astype(BF16)

    def o_copy(t, slot):
        return remote(oall.at[tp], oall.at[slot], oss.at[t], ors.at[slot], "tp", t)

    def o_out(t):
        return pltpu.make_async_copy(
            oall.at[t], out.at[pl.ds(pl.multiple_of(t * R, R), R)], outs.at[t]
        )

    others(TP, tp, lambda t: o_copy(t, tp).start())
    o_out(tp).start()

    def o_in(t):
        remote(oall.at[tp], oall.at[t], oss.at[t], ors.at[t], "tp", t).wait_recv()
        o_out(t).start()

    others(TP, tp, o_in)
    each(TP, lambda t: o_out(t).wait())

    @pl.when(me < S - 1)
    def _():
        def sent(b):
            @pl.when(b <= me)
            def _():
                for c in kv_copies(b, False):
                    c.wait_send()
                each(pieces, lambda p: h_right(p, b).wait_send())

        each(S, sent)

    @pl.when(me > 0)
    def _():
        def sent(b):
            @pl.when(b >= me)
            def _():
                each(pieces, lambda p: h_left(p, b).wait_send())

        each(S, sent)

    def sp_sent(j):
        n1_copy(j, me).wait_send()
        z_copy(j, me).wait_send()
        each(pieces, lambda p: g_copy(p, j, j, right).wait_send())

    others(S, me, sp_sent)

    def tp_sent(t):
        hp_copy(t, tp).wait_send()
        o_copy(t, tp).wait_send()

        def inner(s):
            n2_copy(t, tp, s).wait_send()
            up_copy(t, tp, s).wait_send()

        each(S, inner)

    others(TP, tp, tp_sent)


def solution(mesh):
    S, TP = mesh.shape["sp"], mesh.shape["tp"]

    def shards(q, k, v, lg, res, ow, mg, fg, og, gw, uw, dw):
        T, H = lg.shape
        hw = q.shape[1]
        D = res.shape[1]
        C, U = gw.shape
        R = T // TP
        pieces = max([p for p in range(1, MOST_PIECES + 1) if U % (128 * p) == 0], default=1)
        W = U // pieces
        pad = -H % 8
        lgt = jnp.pad(lg.astype(F32).T, ((0, pad), (0, 0)))
        vm = pl.BlockSpec(memory_space=pltpu.VMEM)
        hb = pl.BlockSpec(memory_space=pl.ANY)
        dma = pltpu.SemaphoreType.DMA
        return pl.pallas_call(
            functools.partial(kernel, S, TP, H, pieces),
            out_shape=jax.ShapeDtypeStruct((T, D), BF16),
            in_specs=[vm] * 7 + [hb] * 5,
            out_specs=hb,
            scratch_shapes=[
                pltpu.VMEM((S, T, hw), BF16),
                pltpu.VMEM((S, T, hw), BF16),
                pltpu.VMEM((S,) + lgt.shape, F32),
                pltpu.VMEM((H, T, hw // H), F32),
                pltpu.VMEM((H, T, hw // H), F32),
                pltpu.VMEM(ow.shape, BF16),
                pltpu.VMEM(gw.shape, BF16),
                pltpu.VMEM(uw.shape, BF16),
                pltpu.VMEM(dw.shape, BF16),
                pltpu.VMEM((R, D), BF16),
                pltpu.VMEM((TP, R, D), BF16),
                pltpu.VMEM((TP, R, D), BF16),
                pltpu.VMEM((R, D), F32),
                pltpu.VMEM((R, C), F32),
                pltpu.VMEM((S, R, C), BF16),
                pltpu.VMEM((TP, S, R, C), BF16),
                pltpu.VMEM((2, T, W), F32),
                pltpu.VMEM((pieces, S, 2, T, W), BF16),
                pltpu.VMEM((pieces, S + 1, 2, T, W), BF16),
                pltpu.VMEM((pieces, S, T, W), BF16),
                pltpu.VMEM((TP, S, R, C), BF16),
                pltpu.VMEM((TP, S, R, C), BF16),
                pltpu.VMEM((S, R, C), BF16),
                pltpu.VMEM((S, R, C), BF16),
                pltpu.VMEM((TP, R, D), BF16),
                dma((5,)),
                dma((S, 3)),
                dma((S, 3)),
                dma((TP,)),
                dma((TP,)),
                dma((S,)),
                dma((S,)),
                dma((TP, S)),
                dma((TP, S)),
                dma((pieces, S)),
                dma((pieces, S + 1)),
                dma((pieces, S)),
                dma((pieces, S)),
                dma((pieces, S)),
                dma((TP, S)),
                dma((TP, S)),
                dma((S,)),
                dma((S,)),
                dma((TP,)),
                dma((TP,)),
                dma((TP,)),
            ],
            compiler_params=pltpu.CompilerParams(
                collective_id=0, has_side_effects=True, vmem_limit_bytes=67043328 - 2**20
            ),
        )(q, k, v, lgt, mg[None], fg[None], og[None], res, ow, gw, uw, dw)

    placed = (
        P(("grp", "sp"), "tp"),
        P(("grp", "sp"), "tp"),
        P(("grp", "sp"), "tp"),
        P(("grp", "sp"), "tp"),
        P(("grp", "sp"), None),
        P("tp", None),
        P(),
        P(),
        P(),
        P("sp", "tp"),
        P("sp", "tp"),
        P("sp", "tp"),
    )
    return jax.shard_map(
        shards, mesh=mesh, in_specs=placed, out_specs=P(("grp", "sp"), None), check_vma=False
    )
```
